32 devices in a mesh: fs: 8 (over z, x), tp: 4 (over y, core).
Axes of the slice: x: 2, y: 2, z: 4, core: 2. Of those that a mesh axis runs over, the one named last changes fastest.
Arguments:
- tokens: bfloat16 [768, 4, 2048], P(None, 'tp'), may hold values from -6 to 6
- norm_gain: float32 [2048], P('fs'), may hold values from 0.1 to 1.9
- gate_weight: float32 [8, 2048, 4096], P(None, 'fs', 'tp'), may hold values from -0.125 to 0.125
- up_weight: float32 [8, 2048, 4096], P(None, 'fs', 'tp'), may hold values from -0.125 to 0.125
- down_weight: float32 [8, 2048, 4096], P(None, 'fs', 'tp'), may hold values from -0.09375 to 0.09375
- expert_ids: int32 [768, 4, 2], P(None, 'tp'), may hold values from 0 to 7, all different within a row
- expert_mix: float32 [768, 4, 2], P(None, 'tp'), may hold values from 0.2 to 1
Outputs:
- gate_serve: bfloat16 [8, 2048, 4096], P(None, None, 'fs')
- up_serve: bfloat16 [8, 2048, 4096], P(None, None, 'fs')
- down_serve: bfloat16 [8, 2048, 4096], P(None, None, 'fs')
- mixed: bfloat16 [768, 4, 2048], P('fs', 'tp')
The draws below stay inside these ranges and needn't reach their ends.
Inputs may be any that keep to these rules, and one draw needn't show every extreme that they name: `expert_ids`: each token names two different experts.
All inputs are finite; a program needn't handle non-finite values.
Results may differ from the reference program's by a relative error of at most 0.0082.
Values may be sent and summed in bfloat16 or wider, within the bound.
A program may use at most 192 MiB of HBM per device.

```python
import jax
import jax.numpy as jnp
from jax import lax

D = 2048
FF = 4096
EXPERTS = 8
ROWS = 768
N_TP = 4


def shard_levels(rng, shape, pieces, smallest, top_value):
    gain, own = 1.0, jax.random.fold_in(rng, 6)
    for axis_at, parts in pieces:
        heights = jnp.exp(jax.random.uniform(jax.random.fold_in(own, axis_at), (parts,), jnp.float32, smallest / len(pieces), top_value / len(pieces)))
        gain = gain * jnp.repeat(heights, shape[axis_at] // parts).reshape([-1 if axis == axis_at else 1 for axis in range(len(shape))])
    return gain


def picks_of(key, rows, count, top, lift):
    order = jax.random.permutation(jax.random.fold_in(key, 1), count)
    pull = order
    for power in range(3):
        pull = pull * pull // count
    pull = pull * lift // count
    tickets = jax.random.randint(jax.random.fold_in(key, 2), (rows, count), 0, 4096) + pull
    fixed_rows = jax.random.permutation(jax.random.fold_in(key, 3), rows)[jnp.arange(count) % rows]
    tickets = jnp.where(jnp.arange(rows)[:, None] == fixed_rows[None, :], 1 << 14, tickets)
    priority = tickets * count + jnp.arange(count)
    return lax.top_k(priority.astype(jnp.int32), top)[1].astype(jnp.int32)


def normal_values(rng, dims, deviation, reach, pieces=(), held_as=jnp.bfloat16):
    entries = jax.random.normal(rng, dims, jnp.float32) * deviation
    if len(pieces) > 0:
        entries = shard_levels(rng, dims, pieces, -0.22, 0.18) * entries
    return jnp.clip(entries, min=-reach, max=reach).astype(held_as)


def setup_inputs(seed: int = 0) -> dict:
    key_of = jax.random.split(jax.random.key(seed), 8)
    tokens = normal_values(key_of[0], (ROWS, N_TP, D), 1.0, 6.0, ((1, 4),))
    norm_gain = jnp.clip(1.0 + 0.18 * jax.random.normal(key_of[1], (D,), jnp.float32), 0.1, 1.9)
    gate_weight = normal_values(key_of[2], (EXPERTS, D, FF), D ** -0.5, 0.125, ((1, 8), (2, 4)), jnp.float32)
    up_weight = normal_values(key_of[3], (EXPERTS, D, FF), D ** -0.5, 0.125, ((1, 8), (2, 4)), jnp.float32)
    down_weight = normal_values(key_of[4], (EXPERTS, D, FF), FF ** -0.5, 0.09375, ((1, 8), (2, 4)), jnp.float32)
    expert_ids = picks_of(key_of[5], ROWS * N_TP, EXPERTS, 2, 0).reshape((ROWS, N_TP, 2))
    expert_mix = jnp.clip(0.2 + 0.8 * jax.random.uniform(key_of[6], (ROWS, N_TP, 2), jnp.float32) ** shard_levels(key_of[6], (ROWS, N_TP, 2), ((1, 4),), -0.2, 0.2), 0.2, 1.0)
    return dict(tokens=tokens, norm_gain=norm_gain, gate_weight=gate_weight, up_weight=up_weight, down_weight=down_weight, expert_ids=expert_ids, expert_mix=expert_mix)


norm_eps = 1e-05

def reference(tokens, norm_gain, gate_weight, up_weight, down_weight, expert_ids, expert_mix):
    gate_serve = (gate_weight * norm_gain[None, :, None]).astype(jnp.bfloat16)
    up_serve = (up_weight * norm_gain[None, :, None]).astype(jnp.bfloat16)
    down_serve = down_weight.astype(jnp.bfloat16)
    token_rows = tokens.reshape(-1, D).astype(jnp.float32)
    row_mean = lax.optimization_barrier(jnp.mean(token_rows, axis=1, keepdims=True))
    centered = token_rows - row_mean
    variance = lax.optimization_barrier(jnp.mean(centered * centered, axis=1, keepdims=True))
    normed = (centered * lax.rsqrt(variance + norm_eps)).astype(jnp.bfloat16)
    route_ids = expert_ids.reshape(-1, 2)
    route_mix = expert_mix.reshape(-1, 2)
    expert_iota = jnp.arange(EXPERTS, dtype=jnp.int32)
    expert_gates = lax.optimization_barrier(jnp.sum((route_ids[:, :, None] == expert_iota[None, None, :]).astype(jnp.float32) * route_mix[:, :, None], axis=1))

    def add_expert(running, weights_now):
        gate_mat, up_mat, down_mat, gate_col = weights_now
        gate_act = jnp.dot(normed, gate_mat, preferred_element_type=jnp.float32)
        up_act = jnp.dot(normed, up_mat, preferred_element_type=jnp.float32)
        hidden = (jax.nn.silu(gate_act) * up_act * gate_col[:, None]).astype(jnp.bfloat16)
        product = lax.dot_general(hidden, down_mat, (((1,), (1,)), ((), ())), preferred_element_type=jnp.float32)
        return (running + product, None)
    start_sum = jnp.zeros((token_rows.shape[0], D), jnp.float32)
    summed, _ = lax.scan(add_expert, start_sum, (gate_serve, up_serve, down_serve, expert_gates.T))
    mixed = summed.astype(jnp.bfloat16).reshape(ROWS, N_TP, D)
    return (gate_serve, up_serve, down_serve, mixed)
```

```python
import functools

import jax
import jax.numpy as jnp
from jax import lax
from jax.experimental import pallas as pl
from jax.experimental.pallas import tpu as pltpu
from jax.sharding import PartitionSpec as P

norm_eps = 1e-05
MESH = pl.DeviceIdType.MESH


PARTS = 2
LEAD = 4
LAG = 10
GAP = 2


def exchange_kernel(n_fs, n_tp, tokens, gain, ids, mix, gate_in, up_in, down_in, gate_out, up_out, down_out, relay_buf,
                    partial, cast, raw, normed, gates, held, total, hop_send, hop_recv, own_send, pass_send, core_send,
                    side_send, land, load, fetch):
    raws, outs = (gate_in, up_in, down_in), (gate_out, up_out, down_out)
    experts, rows, columns = gate_in.shape
    per = n_fs // n_tp
    unit = columns // per
    sub = rows // PARTS
    chunks = experts * PARTS
    half = n_fs // 2
    f, t = lax.axis_index("fs"), lax.axis_index("tp")
    mate = t + 1 - 2 * lax.rem(t, 2)
    side = lax.rem(t + 2, n_tp)
    own = lax.div(f, per)
    own_mate = own + 1 - 2 * lax.rem(own, 2)
    near = t == own_mate
    far = t == lax.rem(own_mate + 2, n_tp)
    inner = lax.div(f, half) == lax.div(t, 2)
    cross = pl.ds((1 - lax.div(f, half)) * half, half)

    def place(j):
        return lax.div(j, PARTS), pl.ds(pl.multiple_of(lax.rem(j, PARTS) * sub, sub), sub)

    def hop(k, j):
        e, now = place(j)
        return pltpu.make_async_remote_copy(
            src_ref=cast.at[k, e, now], dst_ref=relay_buf.at[k - 1, e, now], send_sem=hop_send.at[k - 1, j],
            recv_sem=hop_recv.at[k - 1, j], device_id=(f, side), device_id_type=MESH)

    def straight(k, j, h):
        e, now = place(j)
        return pltpu.make_async_remote_copy(
            src_ref=cast.at[k, e, now, pl.ds(h * unit, unit)], dst_ref=outs[k].at[e, f, now],
            send_sem=own_send.at[k, j, h], recv_sem=land.at[k, j], device_id=(t * per + h, mate), device_id_type=MESH)

    def relayed(k, j, h):
        e, now = place(j)
        return pltpu.make_async_remote_copy(
            src_ref=relay_buf.at[k - 1, e, now, pl.ds(h * unit, unit)], dst_ref=outs[k].at[e, f, now],
            send_sem=pass_send.at[k - 1, j, h], recv_sem=land.at[k, j],
            device_id=(side * per + h, mate), device_id_type=MESH)

    def to_mate(k, j):
        e, now = place(j)
        return pltpu.make_async_remote_copy(
            src_ref=outs[k].at[e, :, now], dst_ref=outs[k].at[e, :, now], send_sem=core_send.at[k, j],
            recv_sem=land.at[k, j], device_id=(f, mate), device_id_type=MESH)

    def to_side(k, j):
        e, now = place(j)
        which = cross if k == 2 else slice(None)
        return pltpu.make_async_remote_copy(
            src_ref=outs[k].at[e, which, now], dst_ref=outs[k].at[e, which, now], send_sem=side_send.at[k, j],
            recv_sem=land.at[k, j], device_id=(f, side), device_id_type=MESH)

    def landed(k, j):
        to_mate(k, j).wait_recv()

    def reads(j, slot):
        e, now = place(j)
        return [pltpu.make_async_copy(raws[k].at[e, now], raw.at[slot, k], fetch.at[slot, k]) for k in range(3)]

    def rounded(j):
        slot = lax.rem(j, 2)
        e, now = place(j)

        @pl.when(j + 1 < chunks)
        def _():
            for copy in reads(j + 1, 1 - slot):
                copy.start()

        for copy in reads(j, slot):
            copy.wait()
        scale = gain[now, :]
        cast[2, e, now, :] = raw[slot, 2].astype(jnp.bfloat16)
        cast[1, e, now, :] = (raw[slot, 1] * scale).astype(jnp.bfloat16)
        cast[0, e, now, :] = (raw[slot, 0] * scale).astype(jnp.bfloat16)

    def sent(j):
        hop(2, j).start()
        hop(1, j).start()
        for k in (0, 1):
            for h in range(per):
                straight(k, j, h).start()

        @pl.when(inner)
        def _():
            for h in range(per):
                straight(2, j, h).start()

    def opened(j):
        @pl.when(j < chunks)
        def _():
            rounded(j)

        @pl.when((j >= 1) & (j < chunks + 1))
        def _():
            sent(j - 1)

    def loads(j):
        e, now = place(j)
        return [pltpu.make_async_copy(outs[k].at[e, :, now], held.at[k, :, now], load.at[k, lax.rem(j, PARTS)])
                for k in range(3)]

    tall = normed.shape[0] // 2
    deep = n_fs * rows

    def compute(e):
        for r in range(PARTS):
            for copy in loads(e * PARTS + r):
                copy.wait()

        def some_rows(i, carry):
            now = pl.ds(pl.multiple_of(i * tall, tall), tall)
            fed = normed[now, :]
            gate_act = jnp.dot(fed, held[0].reshape(deep, unit), preferred_element_type=jnp.float32)
            up_act = jnp.dot(fed, held[1].reshape(deep, unit), preferred_element_type=jnp.float32)
            lanes = lax.broadcasted_iota(jnp.int32, (tall, gates.shape[1]), 1)
            gate = jnp.sum(jnp.where(lanes == e, gates[now, :], 0.0), axis=1, keepdims=True)
            hidden = gate_act / (1.0 + jnp.exp(-gate_act)) * up_act * gate
            total[now, :] += lax.dot_general(
                hidden.astype(jnp.bfloat16), held[2].reshape(deep, unit), (((1,), (1,)), ((), ())),
                preferred_element_type=jnp.float32)
            return carry

        lax.fori_loop(0, 2, some_rows, 0)

    for copy in reads(0, 0):
        copy.start()

    def early(j, carry):
        opened(j)
        return carry

    lax.fori_loop(0, LEAD + 1, early, 0)

    fair = normed.shape[0] // 8

    def norm_rows(i):
        now = pl.ds(pl.multiple_of(i * fair, fair), fair)
        values = tokens[now, :].astype(jnp.float32)
        centered = values - jnp.mean(values, axis=1, keepdims=True)
        variance = jnp.mean(centered * centered, axis=1, keepdims=True)
        normed[now, :] = (centered * lax.rsqrt(variance + norm_eps)).astype(jnp.bfloat16)
        total[now, :] = jnp.zeros((fair, total.shape[1]), jnp.float32)

    expert = lax.broadcasted_iota(jnp.int32, (128, ids.shape[1]), 0)
    chosen = sum(jnp.where(ids[c:c + 1, :] == expert, mix[c:c + 1, :], 0.0) for c in range(2))
    gates[...] = chosen.T

    def step(s, carry):
        opened(s + LEAD + 1)

        @pl.when(s < chunks)
        def _():
            for k in (2, 1):
                hop(k, s).wait_recv()
                for h in range(per):
                    relayed(k, s, h).start()

        @pl.when(s < 8)
        def _():
            norm_rows(s)

        @pl.when((s >= LAG) & (s < chunks + LAG))
        def _():
            j = s - LAG

            @pl.when(near)
            def _():
                landed(0, j)
                to_side(0, j).start()
                to_mate(0, j).start()
                landed(1, j)
                to_mate(1, j).start()

            @pl.when(far)
            def _():
                landed(2, j)
                to_side(2, j).start()
                to_mate(2, j).start()
                landed(1, j)
                to_mate(1, j).start()

        @pl.when(s >= LAG + GAP)
        def _():
            j = s - LAG - GAP

            @pl.when(near)
            def _():
                landed(2, j)
                to_mate(2, j).start()

            @pl.when(far)
            def _():
                landed(0, j)
                to_mate(0, j).start()

            @pl.when(jnp.logical_not(near | far))
            def _():
                for k in range(3):
                    landed(k, j)

            for copy in loads(j):
                copy.start()

            @pl.when(lax.rem(j, PARTS) == PARTS - 1)
            def _():
                compute(lax.div(j, PARTS))

        return carry

    lax.fori_loop(0, chunks + LAG + GAP, step, 0)
    partial[...] = total[...].astype(jnp.bfloat16)

    def drain(j, carry):
        for k in (1, 2):
            hop(k, j).wait_send()
            for h in range(per):
                relayed(k, j, h).wait_send()
        for k in (0, 1):
            for h in range(per):
                straight(k, j, h).wait_send()

        @pl.when(inner)
        def _():
            for h in range(per):
                straight(2, j, h).wait_send()

        @pl.when(near | far)
        def _():
            for k in range(3):
                to_mate(k, j).wait_send()

        @pl.when(near)
        def _():
            to_side(0, j).wait_send()

        @pl.when(far)
        def _():
            to_side(2, j).wait_send()

        return carry

    lax.fori_loop(0, chunks, drain, 0)


def exchange(n_fs, n_tp, tokens, gain, ids, mix, weights):
    experts, rows, columns = weights[0].shape
    per = n_fs // n_tp
    unit = columns // per
    count, width = tokens.shape
    chunks = experts * PARTS
    serve = jax.ShapeDtypeStruct((experts, n_fs, rows, unit), jnp.bfloat16)
    relay = jax.ShapeDtypeStruct((2, experts, rows, columns), jnp.bfloat16)
    dma = pltpu.SemaphoreType.DMA
    outs = pl.pallas_call(
        functools.partial(exchange_kernel, n_fs, n_tp),
        out_shape=(serve, serve, serve, relay, jax.ShapeDtypeStruct(tokens.shape, jnp.bfloat16)),
        in_specs=[pl.BlockSpec(memory_space=pltpu.VMEM)] * 4 + [pl.BlockSpec(memory_space=pl.ANY)] * 3,
        out_specs=[pl.BlockSpec(memory_space=pl.ANY)] * 4 + [pl.BlockSpec(memory_space=pltpu.VMEM)],
        scratch_shapes=[
            pltpu.VMEM((3, experts, rows, columns), jnp.bfloat16),
            pltpu.VMEM((2, 3, rows // PARTS, columns), jnp.float32),
            pltpu.VMEM((count, width), jnp.bfloat16),
            pltpu.VMEM((count, 128), jnp.float32),
            pltpu.VMEM((3, n_fs, rows, unit), jnp.bfloat16),
            pltpu.VMEM((count, width), jnp.float32),
            dma((2, chunks)),
            dma((2, chunks)),
            dma((3, chunks, per)),
            dma((2, chunks, per)),
            dma((3, chunks)),
            dma((3, chunks)),
            dma((3, chunks)),
            dma((3, PARTS)),
            dma((2, 3)),
        ],
        compiler_params=pltpu.CompilerParams(has_side_effects=True, vmem_limit_bytes=60 * 1024 * 1024),
    )(tokens, gain, ids, mix, *weights)
    return tuple(out.reshape(experts, n_fs * rows, unit) for out in outs[:3]) + (outs[4],)


def copy_kernel(*refs):
    half = len(refs) // 2
    for source, target in zip(refs[:half], refs[half:]):
        target[...] = source[...]


def copied(arrays):
    experts, deep, unit = arrays[0].shape
    block = pl.BlockSpec((1, deep, unit), lambda e: (e, 0, 0))
    return pl.pallas_call(
        copy_kernel,
        grid=(experts,),
        out_shape=tuple(jax.ShapeDtypeStruct(a.shape, a.dtype) for a in arrays),
        in_specs=[block] * len(arrays),
        out_specs=[block] * len(arrays),
        cost_estimate=pl.CostEstimate(flops=0, bytes_accessed=4 * len(arrays) * arrays[0].size, transcendentals=0),
        compiler_params=pltpu.CompilerParams(vmem_limit_bytes=40 * 1024 * 1024),
    )(*arrays)


def collective_exchange(blocks):
    regrouped = [lax.all_to_all(b, "tp", split_axis=0, concat_axis=2, tiled=True) for b in blocks]
    unit_split = [lax.all_to_all(b, "fs", split_axis=2, concat_axis=1, tiled=True) for b in regrouped]
    return tuple(lax.all_gather(b, "tp", axis=0, tiled=True) for b in unit_split)


def expert_layer(normed, expert_gates, gate_serve, up_serve, down_serve):
    gate_act = jnp.einsum("rd,edf->ref", normed, gate_serve, preferred_element_type=jnp.float32)
    up_act = jnp.einsum("rd,edf->ref", normed, up_serve, preferred_element_type=jnp.float32)
    hidden = (jax.nn.silu(gate_act) * up_act * expert_gates[:, :, None]).astype(jnp.bfloat16)
    return jnp.einsum("ref,edf->rd", hidden, down_serve, preferred_element_type=jnp.float32).astype(jnp.bfloat16)


def sum_parts(parts, n_fs):
    if n_fs > 8:
        parts = lax.all_to_all(parts, "fs", split_axis=0, concat_axis=0, tiled=True)
        return jnp.sum(parts.astype(jnp.float32), axis=0)
    f = lax.axis_index("fs")
    got = [lax.dynamic_index_in_dim(parts, f, 0, keepdims=False)]
    for j in range(1, n_fs):
        mine = lax.dynamic_index_in_dim(parts, lax.rem(f + j, n_fs), 0, keepdims=False)
        got.append(lax.ppermute(mine, "fs", [(i, (i + j) % n_fs) for i in range(n_fs)]))
    return sum(g.astype(jnp.float32) for g in got)


def local(tokens, norm_gain, gate_weight, up_weight, down_weight, expert_ids, expert_mix):
    n_fs, n_tp = lax.axis_size("fs"), lax.axis_size("tp")
    width = tokens.shape[2]
    token_rows = tokens.reshape(-1, width)
    count = token_rows.shape[0]
    route_ids = expert_ids.reshape(-1, 2)
    route_mix = expert_mix.reshape(-1, 2)
    rows, columns = gate_weight.shape[1:]
    unit = columns * n_tp // n_fs
    whole = count % 128 == 0 and n_fs % 2 == 0 and rows % (16 * PARTS) == 0
    if n_tp == 4 and n_fs % n_tp == 0 and unit % 128 == 0 and whole:
        gate_serve, up_serve, down_serve, partial = exchange(
            n_fs, n_tp, token_rows, norm_gain[:, None], route_ids.T, route_mix.T, (gate_weight, up_weight, down_weight))
        gate_serve, up_serve, down_serve = copied((gate_serve, up_serve, down_serve))
    else:
        blocks = (
            (gate_weight * norm_gain[None, :, None]).astype(jnp.bfloat16),
            (up_weight * norm_gain[None, :, None]).astype(jnp.bfloat16),
            down_weight.astype(jnp.bfloat16),
        )
        values = token_rows.astype(jnp.float32)
        centered = values - jnp.mean(values, axis=1, keepdims=True)
        variance = jnp.mean(centered * centered, axis=1, keepdims=True)
        normed = (centered * lax.rsqrt(variance + norm_eps)).astype(jnp.bfloat16)
        expert_iota = jnp.arange(gate_weight.shape[0], dtype=jnp.int32)
        chosen = (route_ids[:, :, None] == expert_iota[None, None, :]).astype(jnp.float32)
        expert_gates = jnp.sum(chosen * route_mix[:, :, None], axis=1)
        gate_serve, up_serve, down_serve = collective_exchange(blocks)
        partial = expert_layer(normed, expert_gates, gate_serve, up_serve, down_serve)
    own_rows = count // n_fs
    summed = sum_parts(partial.reshape(n_fs, own_rows, width), n_fs)
    mixed = summed.astype(jnp.bfloat16).reshape(own_rows, 1, width)
    return (gate_serve, up_serve, down_serve, mixed)


def solution(mesh):
    return jax.shard_map(
        local,
        mesh=mesh,
        in_specs=(
            P(None, "tp", None),
            P("fs"),
            P(None, "fs", "tp"),
            P(None, "fs", "tp"),
            P(None, "fs", "tp"),
            P(None, "tp", None),
            P(None, "tp", None),
        ),
        out_specs=(
            P(None, None, "fs"),
            P(None, None, "fs"),
            P(None, None, "fs"),
            P("fs", "tp", None),
        ),
        check_vma=False,
    )
```

```python
import functools

import jax
import jax.numpy as jnp
from jax import lax
from jax.experimental import pallas as pl
from jax.experimental.pallas import tpu as pltpu
from jax.sharding import PartitionSpec as P

norm_eps = 1e-05
MESH = pl.DeviceIdType.MESH


STRIPS = 8
LEAD = 2
LAG = 4
GAP = 1
NORM_STEPS = 4


def exchange_kernel(n_fs, n_tp, tokens, gain, ids, mix, gate_in, up_in, down_in, stage, relay_buf, *rest):
    zs = n_fs // 2
    sums, rest = rest[:zs], rest[zs:]
    (scale, cast, raw, raw_down, normed, gates, hid, held, held_down, strip_sum, leaving, staying, arriving,
     hop_send, hop_recv, own_send, pass_send, core_send, side_send, land, load, load_down, fetch, fetch_down,
     pair_send, pair_recv) = rest
    experts, rows, columns = gate_in.shape
    per = n_fs // n_tp
    unit = columns // per
    strip = rows // STRIPS
    chunks = experts + STRIPS
    half = n_fs // 2
    f, t = lax.axis_index("fs"), lax.axis_index("tp")
    mate = t + 1 - 2 * lax.rem(t, 2)
    side = lax.rem(t + 2, n_tp)
    own = lax.div(f, per)
    own_mate = own + 1 - 2 * lax.rem(own, 2)
    near = t == own_mate
    far = t == lax.rem(own_mate + 2, n_tp)
    inner = lax.div(f, half) == lax.div(t, 2)
    cross = pl.ds((1 - lax.div(f, half)) * half, half)
    every = pl.ds(0, n_fs)
    both = pl.ds(0, per)
    x = lax.rem(f, 2)
    z = lax.div(f, 2)

    third = rows // 48 * 16
    odd = rows - 2 * third
    few = experts // 3
    many = (experts - few) // 2
    wide = ((0, 0, 0, odd), (0, 1, odd, third), (0, 2, odd + third, third),
            (1, 0, 0, third), (1, 1, third, third), (1, 2, 2 * third, odd))
    slim = ((2, 0, 0, many), (2, 1, many, few), (2, 2, many + few, experts - many - few))

    def at(p, j):
        k, _, first, size = p
        if k < 2:
            return (k, j, pl.ds(first, size))
        return (k, pl.ds(first, size), pl.ds(pl.multiple_of(j * strip, strip), strip))

    def split(p, j, which):
        index = at(p, j)
        return index[:2] + (which,) + index[2:]

    def name(p):
        return 3 * p[0] + p[1]

    def on_stage(p, j, which):
        return stage.at[split(p, j, which)]

    def hop(p, j):
        return pltpu.make_async_remote_copy(
            src_ref=cast.at[split(p, j, both)], dst_ref=relay_buf.at[split(p, j, both)], send_sem=hop_send.at[name(p), j],
            recv_sem=hop_recv.at[name(p), j], device_id=(f, side), device_id_type=MESH)

    def straight(p, j, h):
        return pltpu.make_async_remote_copy(
            src_ref=cast.at[split(p, j, h)], dst_ref=on_stage(p, j, f),
            send_sem=own_send.at[name(p), j, h], recv_sem=land.at[name(p), j],
            device_id=(t * per + h, mate), device_id_type=MESH)

    def relayed(p, j, h):
        return pltpu.make_async_remote_copy(
            src_ref=relay_buf.at[split(p, j, h)], dst_ref=on_stage(p, j, f),
            send_sem=pass_send.at[name(p), j, h], recv_sem=land.at[name(p), j],
            device_id=(side * per + h, mate), device_id_type=MESH)

    def to_mate(p, j):
        return pltpu.make_async_remote_copy(
            src_ref=on_stage(p, j, every), dst_ref=on_stage(p, j, every), send_sem=core_send.at[name(p), j],
            recv_sem=land.at[name(p), j], device_id=(f, mate), device_id_type=MESH)

    def to_side(p, j):
        which = cross if p[1] == 2 else every
        return pltpu.make_async_remote_copy(
            src_ref=on_stage(p, j, which), dst_ref=on_stage(p, j, which), send_sem=side_send.at[name(p), j],
            recv_sem=land.at[name(p), j], device_id=(f, side), device_id_type=MESH)

    def landed(p, j):
        to_mate(p, j).wait_recv()

    def each(j, act):
        @pl.when((j >= 0) & (j < experts))
        def _():
            act(wide, j, j)

        if act is pushed_now:
            return

        @pl.when((j >= experts) & (j < chunks))
        def _():
            act(slim, j - experts, j)

    def reads(group, j, at_j):
        slot = lax.rem(at_j, 2)
        if group is wide:
            return [pltpu.make_async_copy(ref.at[j], raw.at[slot, k], fetch.at[slot, k])
                    for k, ref in enumerate((gate_in, up_in))]
        now = pl.ds(pl.multiple_of(j * strip, strip), strip)
        return [pltpu.make_async_copy(down_in.at[:, now], raw_down.at[slot], fetch_down.at[slot])]

    def ask(group, j, at_j):
        for copy in reads(group, j, at_j):
            copy.start()

    def rounded(group, j, at_j):
        slot = lax.rem(at_j, 2)
        each(at_j + 1, ask)
        for copy in reads(group, j, at_j):
            copy.wait()
        if group is wide:
            for k in range(2):
                for h in range(per):
                    here = raw[slot, k, :, h * unit:(h + 1) * unit]
                    cast[k, j, h] = (here * scale[:, :1]).astype(jnp.bfloat16)
        else:
            now = pl.ds(pl.multiple_of(j * strip, strip), strip)
            for h in range(per):
                cast[2, :, h, now, :] = raw_down[slot, :, :, h * unit:(h + 1) * unit].astype(jnp.bfloat16)

    def by_route(group, *routes):
        return [p for k in range(3) for r in routes for p in group if p[0] == k and p[1] == r]

    def push(group, j):
        for p in by_route(group, 2, 1):
            hop(p, j).start()
        for p in by_route(group, 0, 1):
            for h in range(per):
                straight(p, j, h).start()

        @pl.when(inner)
        def _():
            for p in by_route(group, 2):
                for h in range(per):
                    straight(p, j, h).start()

    def pushed_now(group, j, at_j):
        push([p for p in group if p[0] == 0], j)

    def pushed_later(group, j, at_j):
        push([p for p in group if p[0] > 0], j)

    def passed(group, j, at_j):
        for p in by_route(group, 2, 1):
            hop(p, j).wait_recv()
            for h in range(per):
                relayed(p, j, h).start()

    def spread(group, j, at_j):
        def out_of(first):
            for p in by_route(group, first, 1):
                landed(p, j)
                if p[1] != 1:
                    to_side(p, j).start()
                to_mate(p, j).start()

        @pl.when(near)
        def _():
            out_of(0)

        @pl.when(far)
        def _():
            out_of(2)

    fair = normed.shape[0] // NORM_STEPS

    def norm_rows(i):
        now = pl.ds(pl.multiple_of(i * fair, fair), fair)
        values = tokens[now, :].astype(jnp.float32)
        centered = values - jnp.mean(values, axis=1, keepdims=True)
        variance = jnp.mean(centered * centered, axis=1, keepdims=True)
        normed[now, :] = (centered * lax.rsqrt(variance + norm_eps)).astype(jnp.bfloat16)

    tall = normed.shape[0] // 2
    deep = n_fs * rows
    short = normed.shape[0] // n_fs
    breadth = n_fs * strip

    def fill_hidden(e):
        copies = [pltpu.make_async_copy(stage.at[k, e], held.at[k], load.at[k]) for k in range(2)]
        for copy in copies:
            copy.start()
        for copy in copies:
            copy.wait()

        def some_rows(i, carry):
            now = pl.ds(pl.multiple_of(i * tall, tall), tall)
            fed = normed[now, :]
            gate_act = jnp.dot(fed, held[0].reshape(deep, unit), preferred_element_type=jnp.float32)
            up_act = jnp.dot(fed, held[1].reshape(deep, unit), preferred_element_type=jnp.float32)
            lanes = lax.broadcasted_iota(jnp.int32, (tall, gates.shape[1]), 1)
            gate = jnp.sum(jnp.where(lanes == e, gates[now, :], 0.0), axis=1, keepdims=True)
            hidden = gate_act / (1.0 + jnp.exp(-gate_act)) * up_act * gate
            hid[e, now, :] = hidden.astype(jnp.bfloat16)
            return carry

        lax.fori_loop(0, 2, some_rows, 0)

    def pair(q):
        return pltpu.make_async_remote_copy(
            src_ref=leaving.at[q], dst_ref=arriving.at[q], send_sem=pair_send.at[q], recv_sem=pair_recv.at[q],
            device_id=(f + 1 - 2 * x, t), device_id_type=MESH)

    def merge(q):
        pair(q).wait_recv()
        now = pl.ds(pl.multiple_of(q * breadth, breadth), breadth)
        for ahead in range(zs):
            goal = lax.rem(z + ahead, zs)
            total = staying[q, goal] + arriving[q, goal].astype(jnp.float32)
            sums[ahead][:, now] = total.astype(jnp.bfloat16)

    def sum_strip(q):
        now = pl.ds(pl.multiple_of(q * strip, strip), strip)
        copy = pltpu.make_async_copy(stage.at[2, :, :, now], held_down, load_down)
        copy.start()

        @pl.when(q >= 1)
        def _():
            merge(q - 1)

        copy.wait()

        def some_rows(i, carry):
            now = pl.ds(pl.multiple_of(i * tall, tall), tall)
            acc = jnp.zeros((tall, breadth), jnp.float32)
            for e in range(experts):
                acc += lax.dot_general(
                    hid[e, now, :], held_down[e].reshape(breadth, unit), (((1,), (1,)), ((), ())),
                    preferred_element_type=jnp.float32)
            strip_sum[now, :] = acc
            return carry

        lax.fori_loop(0, 2, some_rows, 0)
        for goal in range(zs):
            theirs = pl.ds(pl.multiple_of((2 * goal + 1 - x) * short, short), short)
            leaving[q, goal] = strip_sum[theirs, :].astype(jnp.bfloat16)
        for goal in range(zs):
            mine = pl.ds(pl.multiple_of((2 * goal + x) * short, short), short)
            staying[q, goal] = strip_sum[mine, :]
        pair(q).start()

    def used(group, j, at_j):
        @pl.when(near)
        def _():
            for p in by_route(group, 2):
                landed(p, j)
                to_mate(p, j).start()

        @pl.when(far)
        def _():
            for p in by_route(group, 0):
                landed(p, j)
                to_mate(p, j).start()

        @pl.when(jnp.logical_not(near | far))
        def _():
            for p in group:
                landed(p, j)

        if group is wide:
            fill_hidden(j)
        else:
            sum_strip(j)

    def opened(j):
        each(j - 1, pushed_later)
        each(j, rounded)
        each(j, pushed_now)

    ask(wide, 0, 0)
    scale[...] = jnp.broadcast_to(gain[...], (128, rows)).T

    def early(j, carry):
        opened(j)
        return carry

    lax.fori_loop(0, LEAD + 1, early, 0)
    expert = lax.broadcasted_iota(jnp.int32, (128, ids.shape[1]), 0)
    chosen = sum(jnp.where(ids[c:c + 1, :] == expert, mix[c:c + 1, :], 0.0) for c in range(2))
    gates[...] = chosen.T

    def step(s, carry):
        opened(s + LEAD + 1)
        each(s, passed)

        @pl.when(s < NORM_STEPS)
        def _():
            norm_rows(s)

        each(s - LAG, spread)
        each(s - LAG - GAP, used)
        return carry

    lax.fori_loop(0, chunks + LAG + GAP, step, 0)
    merge(STRIPS - 1)

    def drain(group):
        def some(j, carry):
            for p in by_route(group, 1, 2):
                hop(p, j).wait_send()
                for h in range(per):
                    relayed(p, j, h).wait_send()
            for p in by_route(group, 0, 1):
                for h in range(per):
                    straight(p, j, h).wait_send()

            @pl.when(inner)
            def _():
                for p in by_route(group, 2):
                    for h in range(per):
                        straight(p, j, h).wait_send()

            @pl.when(near | far)
            def _():
                for p in group:
                    to_mate(p, j).wait_send()

            @pl.when(near)
            def _():
                for p in by_route(group, 0):
                    to_side(p, j).wait_send()

            @pl.when(far)
            def _():
                for p in by_route(group, 2):
                    to_side(p, j).wait_send()

            if group is slim:
                pair(j).wait_send()
            return carry

        return some

    lax.fori_loop(0, experts, drain(wide), 0)
    lax.fori_loop(0, STRIPS, drain(slim), 0)


def exchange(n_fs, n_tp, tokens, gain, ids, mix, weights):
    experts, rows, columns = weights[0].shape
    per = n_fs // n_tp
    unit = columns // per
    count, width = tokens.shape
    zs = n_fs // 2
    short = count // n_fs
    strip = rows // STRIPS
    longest = max(experts, STRIPS)
    serve = jax.ShapeDtypeStruct((3, experts, n_fs, rows, unit), jnp.bfloat16)
    relay = jax.ShapeDtypeStruct((3, experts, per, rows, unit), jnp.bfloat16)
    piece = jax.ShapeDtypeStruct((short, width), jnp.bfloat16)
    dma = pltpu.SemaphoreType.DMA
    vmem = pl.BlockSpec(memory_space=pltpu.VMEM)
    hbm = pl.BlockSpec(memory_space=pl.ANY)
    outs = pl.pallas_call(
        functools.partial(exchange_kernel, n_fs, n_tp),
        out_shape=(serve, relay) + (piece,) * zs,
        in_specs=[vmem] * 4 + [hbm] * 3,
        out_specs=[hbm] * 2 + [vmem] * zs,
        scratch_shapes=[
            pltpu.VMEM((rows, 128), jnp.float32),
            pltpu.VMEM((3, experts, per, rows, unit), jnp.bfloat16),
            pltpu.VMEM((2, 2, rows, columns), jnp.float32),
            pltpu.VMEM((2, experts, strip, columns), jnp.float32),
            pltpu.VMEM((count, width), jnp.bfloat16),
            pltpu.VMEM((count, 128), jnp.float32),
            pltpu.VMEM((experts, count, unit), jnp.bfloat16),
            pltpu.VMEM((2, n_fs, rows, unit), jnp.bfloat16),
            pltpu.VMEM((experts, n_fs, strip, unit), jnp.bfloat16),
            pltpu.VMEM((count, n_fs * strip), jnp.float32),
            pltpu.VMEM((STRIPS, zs, short, n_fs * strip), jnp.bfloat16),
            pltpu.VMEM((STRIPS, zs, short, n_fs * strip), jnp.float32),
            pltpu.VMEM((STRIPS, zs, short, n_fs * strip), jnp.bfloat16),
            dma((9, longest)),
            dma((9, longest)),
            dma((9, longest, per)),
            dma((9, longest, per)),
            dma((9, longest)),
            dma((9, longest)),
            dma((9, longest)),
            dma((2,)),
            dma,
            dma((2, 2)),
            dma((2,)),
            dma((STRIPS,)),
            dma((STRIPS,)),
        ],
        compiler_params=pltpu.CompilerParams(has_side_effects=True, vmem_limit_bytes=60 * 1024 * 1024),
    )(tokens, gain, ids, mix, *weights)
    return outs[0].reshape(3, experts, n_fs * rows, unit), outs[2:]


def copy_kernel(*refs):
    half = len(refs) // 2
    for source, target in zip(refs[:half], refs[half:]):
        target[...] = source[0]


def copied(staged):
    kinds, experts, deep, unit = staged.shape
    block = pl.BlockSpec((1, deep, unit), lambda e: (e, 0, 0))
    return pl.pallas_call(
        copy_kernel,
        grid=(experts,),
        out_shape=(jax.ShapeDtypeStruct(staged.shape[1:], staged.dtype),) * kinds,
        in_specs=[pl.BlockSpec((1, 1, deep, unit), functools.partial(lambda k, e: (k, e, 0, 0), k)) for k in range(kinds)],
        out_specs=[block] * kinds,
        cost_estimate=pl.CostEstimate(flops=0, bytes_accessed=4 * staged.size, transcendentals=0),
        compiler_params=pltpu.CompilerParams(vmem_limit_bytes=40 * 1024 * 1024),
    )(*(staged,) * kinds)


def sum_pieces(pieces, n_fs):
    zs = len(pieces)
    got = [pieces[0]]
    for ahead in range(1, zs):
        got.append(lax.ppermute(pieces[ahead], "fs", [(i, (i + 2 * ahead) % n_fs) for i in range(n_fs)]))
    summed = sum(g.astype(jnp.float32) for g in got).astype(jnp.bfloat16)
    short, width = summed.shape
    return summed.reshape(short, STRIPS, n_fs, -1).transpose(0, 2, 1, 3).reshape(short, width)


def collective_exchange(blocks):
    regrouped = [lax.all_to_all(b, "tp", split_axis=0, concat_axis=2, tiled=True) for b in blocks]
    unit_split = [lax.all_to_all(b, "fs", split_axis=2, concat_axis=1, tiled=True) for b in regrouped]
    return tuple(lax.all_gather(b, "tp", axis=0, tiled=True) for b in unit_split)


def expert_layer(normed, expert_gates, gate_serve, up_serve, down_serve):
    gate_act = jnp.einsum("rd,edf->ref", normed, gate_serve, preferred_element_type=jnp.float32)
    up_act = jnp.einsum("rd,edf->ref", normed, up_serve, preferred_element_type=jnp.float32)
    hidden = (jax.nn.silu(gate_act) * up_act * expert_gates[:, :, None]).astype(jnp.bfloat16)
    return jnp.einsum("ref,edf->rd", hidden, down_serve, preferred_element_type=jnp.float32).astype(jnp.bfloat16)


def sum_parts(parts):
    parts = lax.all_to_all(parts, "fs", split_axis=0, concat_axis=0, tiled=True)
    return jnp.sum(parts.astype(jnp.float32), axis=0)


def local(tokens, norm_gain, gate_weight, up_weight, down_weight, expert_ids, expert_mix):
    n_fs, n_tp = lax.axis_size("fs"), lax.axis_size("tp")
    width = tokens.shape[2]
    token_rows = tokens.reshape(-1, width)
    count = token_rows.shape[0]
    own_rows = count // n_fs
    route_ids = expert_ids.reshape(-1, 2)
    route_mix = expert_mix.reshape(-1, 2)
    experts, rows, columns = gate_weight.shape
    unit = columns * n_tp // n_fs
    cut = experts >= 3 and rows >= 48 and rows % (16 * STRIPS) == 0 and (rows // STRIPS * n_fs) % 128 == 0
    whole = count % (128 * NORM_STEPS // 2) == 0 and own_rows % 16 == 0 and n_fs % 2 == 0
    if n_tp == 4 and n_fs % n_tp == 0 and unit % 128 == 0 and cut and whole:
        staged, pieces = exchange(
            n_fs, n_tp, token_rows, norm_gain[None, :], route_ids.T, route_mix.T, (gate_weight, up_weight, down_weight))
        gate_serve, up_serve, down_serve = copied(staged)
        mixed = sum_pieces(pieces, n_fs)
    else:
        blocks = (
            (gate_weight * norm_gain[None, :, None]).astype(jnp.bfloat16),
            (up_weight * norm_gain[None, :, None]).astype(jnp.bfloat16),
            down_weight.astype(jnp.bfloat16),
        )
        values = token_rows.astype(jnp.float32)
        centered = values - jnp.mean(values, axis=1, keepdims=True)
        variance = jnp.mean(centered * centered, axis=1, keepdims=True)
        normed = (centered * lax.rsqrt(variance + norm_eps)).astype(jnp.bfloat16)
        expert_iota = jnp.arange(experts, dtype=jnp.int32)
        chosen = (route_ids[:, :, None] == expert_iota[None, None, :]).astype(jnp.float32)
        expert_gates = jnp.sum(chosen * route_mix[:, :, None], axis=1)
        gate_serve, up_serve, down_serve = collective_exchange(blocks)
        partial = expert_layer(normed, expert_gates, gate_serve, up_serve, down_serve)
        mixed = sum_parts(partial.reshape(n_fs, own_rows, width)).astype(jnp.bfloat16)
    return (gate_serve, up_serve, down_serve, mixed.reshape(own_rows, 1, width))


def solution(mesh):
    return jax.shard_map(
        local,
        mesh=mesh,
        in_specs=(
            P(None, "tp", None),
            P("fs"),
            P(None, "fs", "tp"),
            P(None, "fs", "tp"),
            P(None, "fs", "tp"),
            P(None, "tp", None),
            P(None, "tp", None),
        ),
        out_specs=(
            P(None, None, "fs"),
            P(None, None, "fs"),
            P(None, None, "fs"),
            P("fs", "tp", None),
        ),
        check_vma=False,
    )
```

```python
import functools

import jax
import jax.numpy as jnp
from jax import lax
from jax.experimental import pallas as pl
from jax.experimental.pallas import tpu as pltpu
from jax.sharding import PartitionSpec as P

norm_eps = 1e-05
MESH = pl.DeviceIdType.MESH


STRIPS = 8
LEAD = 2
LAG = 4
GAP = 1
NORM_STEPS = 4


def exchange_kernel(n_fs, n_tp, tokens, gain, ids, mix, gate_in, up_in, down_in, stage, relay_buf, *rest):
    zs = n_fs // 2
    sums, rest = rest[:zs], rest[zs:]
    (scale, cast, raw, raw_down, normed, gates, hid, held, held_down, strip_sum, leaving, staying, arriving,
     hop_send, hop_recv, own_send, pass_send, core_send, side_send, land, load, load_down, fetch, fetch_down,
     pair_send, pair_recv) = rest
    experts, rows, columns = gate_in.shape
    per = n_fs // n_tp
    unit = columns // per
    strip = rows // STRIPS
    chunks = experts + STRIPS
    half = n_fs // 2
    f, t = lax.axis_index("fs"), lax.axis_index("tp")
    mate = t + 1 - 2 * lax.rem(t, 2)
    side = lax.rem(t + 2, n_tp)
    own = lax.div(f, per)
    own_mate = own + 1 - 2 * lax.rem(own, 2)
    near = t == own_mate
    far = t == lax.rem(own_mate + 2, n_tp)
    inner = lax.div(f, half) == lax.div(t, 2)
    cross = pl.ds((1 - lax.div(f, half)) * half, half)
    every = pl.ds(0, n_fs)
    both = pl.ds(0, per)
    x = lax.rem(f, 2)
    z = lax.div(f, 2)

    mid = rows // 4
    edge = (rows - mid) // 2
    few = experts // 3
    many = (experts - few) // 2
    wide = tuple(p for k in range(2) for p in ((k, 0, 0, edge), (k, 1, edge, mid), (k, 2, edge + mid, edge)))
    slim = ((2, 0, 0, many), (2, 1, many, few), (2, 2, many + few, experts - many - few))

    def at(p, j):
        k, _, first, size = p
        if k < 2:
            return (k, j, pl.ds(first, size))
        return (k, pl.ds(first, size), pl.ds(pl.multiple_of(j * strip, strip), strip))

    def split(p, j, which):
        index = at(p, j)
        return index[:2] + (which,) + index[2:]

    def name(p):
        return 3 * p[0] + p[1]

    def on_stage(p, j, which):
        return stage.at[split(p, j, which)]

    def hop(p, j):
        return pltpu.make_async_remote_copy(
            src_ref=cast.at[split(p, j, both)], dst_ref=relay_buf.at[split(p, j, both)], send_sem=hop_send.at[name(p), j],
            recv_sem=hop_recv.at[name(p), j], device_id=(f, side), device_id_type=MESH)

    def straight(p, j, h):
        return pltpu.make_async_remote_copy(
            src_ref=cast.at[split(p, j, h)], dst_ref=on_stage(p, j, f),
            send_sem=own_send.at[name(p), j, h], recv_sem=land.at[name(p), j],
            device_id=(t * per + h, mate), device_id_type=MESH)

    def relayed(p, j, h):
        return pltpu.make_async_remote_copy(
            src_ref=relay_buf.at[split(p, j, h)], dst_ref=on_stage(p, j, f),
            send_sem=pass_send.at[name(p), j, h], recv_sem=land.at[name(p), j],
            device_id=(side * per + h, mate), device_id_type=MESH)

    def to_mate(p, j):
        return pltpu.make_async_remote_copy(
            src_ref=on_stage(p, j, every), dst_ref=on_stage(p, j, every), send_sem=core_send.at[name(p), j],
            recv_sem=land.at[name(p), j], device_id=(f, mate), device_id_type=MESH)

    def to_side(p, j):
        which = cross if p[1] == 2 else every
        return pltpu.make_async_remote_copy(
            src_ref=on_stage(p, j, which), dst_ref=on_stage(p, j, which), send_sem=side_send.at[name(p), j],
            recv_sem=land.at[name(p), j], device_id=(f, side), device_id_type=MESH)

    def landed(p, j):
        to_mate(p, j).wait_recv()

    def each(j, act):
        @pl.when((j >= 0) & (j < experts))
        def _():
            act(wide, j, j)

        if act is pushed_now:
            return

        @pl.when((j >= experts) & (j < chunks))
        def _():
            act(slim, j - experts, j)

    def reads(group, j, at_j):
        slot = lax.rem(at_j, 2)
        if group is wide:
            return [pltpu.make_async_copy(ref.at[j], raw.at[slot, k], fetch.at[slot, k])
                    for k, ref in enumerate((gate_in, up_in))]
        now = pl.ds(pl.multiple_of(j * strip, strip), strip)
        return [pltpu.make_async_copy(down_in.at[:, now], raw_down.at[slot], fetch_down.at[slot])]

    def ask(group, j, at_j):
        for copy in reads(group, j, at_j):
            copy.start()

    def rounded(group, j, at_j):
        slot = lax.rem(at_j, 2)
        each(at_j + 1, ask)
        for copy in reads(group, j, at_j):
            copy.wait()
        if group is wide:
            for k in range(2):
                for h in range(per):
                    here = raw[slot, k, :, h * unit:(h + 1) * unit]
                    cast[k, j, h] = (here * scale[:, :1]).astype(jnp.bfloat16)
        else:
            now = pl.ds(pl.multiple_of(j * strip, strip), strip)
            for h in range(per):
                cast[2, :, h, now, :] = raw_down[slot, :, :, h * unit:(h + 1) * unit].astype(jnp.bfloat16)

    def by_route(group, *routes):
        return [p for k in range(3) for r in routes for p in group if p[0] == k and p[1] == r]

    def push(group, j):
        for p in by_route(group, 2, 1):
            hop(p, j).start()
        for p in by_route(group, 0, 1):
            for h in range(per):
                straight(p, j, h).start()

        @pl.when(inner)
        def _():
            for p in by_route(group, 2):
                for h in range(per):
                    straight(p, j, h).start()

    def pushed_now(group, j, at_j):
        push([p for p in group if p[0] == 0], j)

    def pushed_later(group, j, at_j):
        push([p for p in group if p[0] > 0], j)

    def passed(group, j, at_j):
        for p in by_route(group, 2, 1):
            hop(p, j).wait_recv()
            for h in range(per):
                relayed(p, j, h).start()

    def spread(group, j, at_j):
        def out_of(first):
            for p in by_route(group, first, 1):
                landed(p, j)
                if p[1] != 1:
                    to_side(p, j).start()
                to_mate(p, j).start()

        @pl.when(near)
        def _():
            out_of(0)

        @pl.when(far)
        def _():
            out_of(2)

    fair = normed.shape[0] // NORM_STEPS

    def norm_rows(i):
        now = pl.ds(pl.multiple_of(i * fair, fair), fair)
        values = tokens[now, :].astype(jnp.float32)
        centered = values - jnp.mean(values, axis=1, keepdims=True)
        variance = jnp.mean(centered * centered, axis=1, keepdims=True)
        normed[now, :] = (centered * lax.rsqrt(variance + norm_eps)).astype(jnp.bfloat16)

    tall = normed.shape[0] // 2
    deep = n_fs * rows
    short = normed.shape[0] // n_fs
    breadth = n_fs * strip

    def fill_hidden(e):
        copies = [pltpu.make_async_copy(stage.at[k, e], held.at[k], load.at[k]) for k in range(2)]
        for copy in copies:
            copy.start()
        for copy in copies:
            copy.wait()

        def some_rows(i, carry):
            now = pl.ds(pl.multiple_of(i * tall, tall), tall)
            fed = normed[now, :]
            gate_act = jnp.dot(fed, held[0].reshape(deep, unit), preferred_element_type=jnp.float32)
            up_act = jnp.dot(fed, held[1].reshape(deep, unit), preferred_element_type=jnp.float32)
            lanes = lax.broadcasted_iota(jnp.int32, (tall, gates.shape[1]), 1)
            gate = jnp.sum(jnp.where(lanes == e, gates[now, :], 0.0), axis=1, keepdims=True)
            hidden = gate_act / (1.0 + jnp.exp(-gate_act)) * up_act * gate
            hid[e, now, :] = hidden.astype(jnp.bfloat16)
            return carry

        lax.fori_loop(0, 2, some_rows, 0)

    def pair(q):
        return pltpu.make_async_remote_copy(
            src_ref=leaving.at[q], dst_ref=arriving.at[q], send_sem=pair_send.at[q], recv_sem=pair_recv.at[q],
            device_id=(f + 1 - 2 * x, t), device_id_type=MESH)

    def merge(q):
        pair(q).wait_recv()
        now = pl.ds(pl.multiple_of(q * breadth, breadth), breadth)
        for ahead in range(zs):
            goal = lax.rem(z + ahead, zs)
            total = staying[q, goal] + arriving[q, goal].astype(jnp.float32)
            sums[ahead][:, now] = total.astype(jnp.bfloat16)

    def sum_strip(q):
        now = pl.ds(pl.multiple_of(q * strip, strip), strip)
        copy = pltpu.make_async_copy(stage.at[2, :, :, now], held_down, load_down)
        copy.start()

        @pl.when(q >= 1)
        def _():
            merge(q - 1)

        copy.wait()

        def some_rows(i, carry):
            now = pl.ds(pl.multiple_of(i * tall, tall), tall)
            acc = jnp.zeros((tall, breadth), jnp.float32)
            for e in range(experts):
                acc += lax.dot_general(
                    hid[e, now, :], held_down[e].reshape(breadth, unit), (((1,), (1,)), ((), ())),
                    preferred_element_type=jnp.float32)
            strip_sum[now, :] = acc
            return carry

        lax.fori_loop(0, 2, some_rows, 0)
        for goal in range(zs):
            theirs = pl.ds(pl.multiple_of((2 * goal + 1 - x) * short, short), short)
            leaving[q, goal] = strip_sum[theirs, :].astype(jnp.bfloat16)
        for goal in range(zs):
            mine = pl.ds(pl.multiple_of((2 * goal + x) * short, short), short)
            staying[q, goal] = strip_sum[mine, :]
        pair(q).start()

    def used(group, j, at_j):
        @pl.when(near)
        def _():
            for p in by_route(group, 2):
                landed(p, j)
                to_mate(p, j).start()

        @pl.when(far)
        def _():
            for p in by_route(group, 0):
                landed(p, j)
                to_mate(p, j).start()

        @pl.when(jnp.logical_not(near | far))
        def _():
            for p in group:
                landed(p, j)

        if group is wide:
            fill_hidden(j)
        else:
            sum_strip(j)

    def opened(j):
        each(j - 1, pushed_later)
        each(j, rounded)
        each(j, pushed_now)

    ask(wide, 0, 0)
    scale[...] = jnp.broadcast_to(gain[...], (128, rows)).T

    def early(j, carry):
        opened(j)
        return carry

    lax.fori_loop(0, LEAD + 1, early, 0)
    expert = lax.broadcasted_iota(jnp.int32, (128, ids.shape[1]), 0)
    chosen = sum(jnp.where(ids[c:c + 1, :] == expert, mix[c:c + 1, :], 0.0) for c in range(2))
    gates[...] = chosen.T

    def step(s, carry):
        opened(s + LEAD + 1)
        each(s, passed)

        @pl.when(s < NORM_STEPS)
        def _():
            norm_rows(s)

        each(s - LAG, spread)
        each(s - LAG - GAP, used)
        return carry

    lax.fori_loop(0, chunks + LAG + GAP, step, 0)
    merge(STRIPS - 1)

    def drain(group):
        def some(j, carry):
            for p in by_route(group, 1, 2):
                hop(p, j).wait_send()
                for h in range(per):
                    relayed(p, j, h).wait_send()
            for p in by_route(group, 0, 1):
                for h in range(per):
                    straight(p, j, h).wait_send()

            @pl.when(inner)
            def _():
                for p in by_route(group, 2):
                    for h in range(per):
                        straight(p, j, h).wait_send()

            @pl.when(near | far)
            def _():
                for p in group:
                    to_mate(p, j).wait_send()

            @pl.when(near)
            def _():
                for p in by_route(group, 0):
                    to_side(p, j).wait_send()

            @pl.when(far)
            def _():
                for p in by_route(group, 2):
                    to_side(p, j).wait_send()

            if group is slim:
                pair(j).wait_send()
            return carry

        return some

    lax.fori_loop(0, experts, drain(wide), 0)
    lax.fori_loop(0, STRIPS, drain(slim), 0)


def exchange(n_fs, n_tp, tokens, gain, ids, mix, weights):
    experts, rows, columns = weights[0].shape
    per = n_fs // n_tp
    unit = columns // per
    count, width = tokens.shape
    zs = n_fs // 2
    short = count // n_fs
    strip = rows // STRIPS
    longest = max(experts, STRIPS)
    serve = jax.ShapeDtypeStruct((3, experts, n_fs, rows, unit), jnp.bfloat16)
    relay = jax.ShapeDtypeStruct((3, experts, per, rows, unit), jnp.bfloat16)
    piece = jax.ShapeDtypeStruct((short, width), jnp.bfloat16)
    dma = pltpu.SemaphoreType.DMA
    vmem = pl.BlockSpec(memory_space=pltpu.VMEM)
    hbm = pl.BlockSpec(memory_space=pl.ANY)
    outs = pl.pallas_call(
        functools.partial(exchange_kernel, n_fs, n_tp),
        out_shape=(serve, relay) + (piece,) * zs,
        in_specs=[vmem] * 4 + [hbm] * 3,
        out_specs=[hbm] * 2 + [vmem] * zs,
        scratch_shapes=[
            pltpu.VMEM((rows, 128), jnp.float32),
            pltpu.VMEM((3, experts, per, rows, unit), jnp.bfloat16),
            pltpu.VMEM((2, 2, rows, columns), jnp.float32),
            pltpu.VMEM((2, experts, strip, columns), jnp.float32),
            pltpu.VMEM((count, width), jnp.bfloat16),
            pltpu.VMEM((count, 128), jnp.float32),
            pltpu.VMEM((experts, count, unit), jnp.bfloat16),
            pltpu.VMEM((2, n_fs, rows, unit), jnp.bfloat16),
            pltpu.VMEM((experts, n_fs, strip, unit), jnp.bfloat16),
            pltpu.VMEM((count, n_fs * strip), jnp.float32),
            pltpu.VMEM((STRIPS, zs, short, n_fs * strip), jnp.bfloat16),
            pltpu.VMEM((STRIPS, zs, short, n_fs * strip), jnp.float32),
            pltpu.VMEM((STRIPS, zs, short, n_fs * strip), jnp.bfloat16),
            dma((9, longest)),
            dma((9, longest)),
            dma((9, longest, per)),
            dma((9, longest, per)),
            dma((9, longest)),
            dma((9, longest)),
            dma((9, longest)),
            dma((2,)),
            dma,
            dma((2, 2)),
            dma((2,)),
            dma((STRIPS,)),
            dma((STRIPS,)),
        ],
        compiler_params=pltpu.CompilerParams(has_side_effects=True, vmem_limit_bytes=60 * 1024 * 1024),
    )(tokens, gain, ids, mix, *weights)
    return outs[0].reshape(3, experts, n_fs * rows, unit), outs[2:]


def copy_kernel(*refs):
    half = len(refs) // 2
    for source, target in zip(refs[:half], refs[half:]):
        target[...] = source[0]


def copied(staged):
    kinds, experts, deep, unit = staged.shape
    block = pl.BlockSpec((1, deep, unit), lambda e: (e, 0, 0))
    return pl.pallas_call(
        copy_kernel,
        grid=(experts,),
        out_shape=(jax.ShapeDtypeStruct(staged.shape[1:], staged.dtype),) * kinds,
        in_specs=[pl.BlockSpec((1, 1, deep, unit), functools.partial(lambda k, e: (k, e, 0, 0), k)) for k in range(kinds)],
        out_specs=[block] * kinds,
        cost_estimate=pl.CostEstimate(flops=0, bytes_accessed=4 * staged.size, transcendentals=0),
        compiler_params=pltpu.CompilerParams(vmem_limit_bytes=40 * 1024 * 1024),
    )(*(staged,) * kinds)


def sum_pieces(pieces, n_fs):
    zs = len(pieces)
    got = [pieces[0]]
    for ahead in range(1, zs):
        got.append(lax.ppermute(pieces[ahead], "fs", [(i, (i + 2 * ahead) % n_fs) for i in range(n_fs)]))
    summed = sum(g.astype(jnp.float32) for g in got).astype(jnp.bfloat16)
    short, width = summed.shape
    return summed.reshape(short, STRIPS, n_fs, -1).transpose(0, 2, 1, 3).reshape(short, width)


def collective_exchange(blocks):
    regrouped = [lax.all_to_all(b, "tp", split_axis=0, concat_axis=2, tiled=True) for b in blocks]
    unit_split = [lax.all_to_all(b, "fs", split_axis=2, concat_axis=1, tiled=True) for b in regrouped]
    return tuple(lax.all_gather(b, "tp", axis=0, tiled=True) for b in unit_split)


def expert_layer(normed, expert_gates, gate_serve, up_serve, down_serve):
    gate_act = jnp.einsum("rd,edf->ref", normed, gate_serve, preferred_element_type=jnp.float32)
    up_act = jnp.einsum("rd,edf->ref", normed, up_serve, preferred_element_type=jnp.float32)
    hidden = (jax.nn.silu(gate_act) * up_act * expert_gates[:, :, None]).astype(jnp.bfloat16)
    return jnp.einsum("ref,edf->rd", hidden, down_serve, preferred_element_type=jnp.float32).astype(jnp.bfloat16)


def sum_parts(parts):
    parts = lax.all_to_all(parts, "fs", split_axis=0, concat_axis=0, tiled=True)
    return jnp.sum(parts.astype(jnp.float32), axis=0)


def local(tokens, norm_gain, gate_weight, up_weight, down_weight, expert_ids, expert_mix):
    n_fs, n_tp = lax.axis_size("fs"), lax.axis_size("tp")
    width = tokens.shape[2]
    token_rows = tokens.reshape(-1, width)
    count = token_rows.shape[0]
    own_rows = count // n_fs
    route_ids = expert_ids.reshape(-1, 2)
    route_mix = expert_mix.reshape(-1, 2)
    experts, rows, columns = gate_weight.shape
    unit = columns * n_tp // n_fs
    cut = experts >= 3 and rows >= 48 and rows % (16 * STRIPS) == 0 and (rows // STRIPS * n_fs) % 128 == 0
    whole = count % (128 * NORM_STEPS // 2) == 0 and own_rows % 16 == 0 and n_fs % 2 == 0
    if n_tp == 4 and n_fs % n_tp == 0 and unit % 128 == 0 and cut and whole:
        staged, pieces = exchange(
            n_fs, n_tp, token_rows, norm_gain[None, :], route_ids.T, route_mix.T, (gate_weight, up_weight, down_weight))
        gate_serve, up_serve, down_serve = copied(staged)
        mixed = sum_pieces(pieces, n_fs)
    else:
        blocks = (
            (gate_weight * norm_gain[None, :, None]).astype(jnp.bfloat16),
            (up_weight * norm_gain[None, :, None]).astype(jnp.bfloat16),
            down_weight.astype(jnp.bfloat16),
        )
        values = token_rows.astype(jnp.float32)
        centered = values - jnp.mean(values, axis=1, keepdims=True)
        variance = jnp.mean(centered * centered, axis=1, keepdims=True)
        normed = (centered * lax.rsqrt(variance + norm_eps)).astype(jnp.bfloat16)
        expert_iota = jnp.arange(experts, dtype=jnp.int32)
        chosen = (route_ids[:, :, None] == expert_iota[None, None, :]).astype(jnp.float32)
        expert_gates = jnp.sum(chosen * route_mix[:, :, None], axis=1)
        gate_serve, up_serve, down_serve = collective_exchange(blocks)
        partial = expert_layer(normed, expert_gates, gate_serve, up_serve, down_serve)
        mixed = sum_parts(partial.reshape(n_fs, own_rows, width)).astype(jnp.bfloat16)
    return (gate_serve, up_serve, down_serve, mixed.reshape(own_rows, 1, width))


def solution(mesh):
    return jax.shard_map(
        local,
        mesh=mesh,
        in_specs=(
            P(None, "tp", None),
            P("fs"),
            P(None, "fs", "tp"),
            P(None, "fs", "tp"),
            P(None, "fs", "tp"),
            P(None, "tp", None),
            P(None, "tp", None),
        ),
        out_specs=(
            P(None, None, "fs"),
            P(None, None, "fs"),
            P(None, None, "fs"),
            P("fs", "tp", None),
        ),
        check_vma=False,
    )
```
